32 devices in a mesh: sp: 16 (over z, y, x), tp: 2 (over core).
Axes of the slice: x: 2, y: 2, z: 4, core: 2. Of those that a mesh axis runs over, the one named last changes fastest.
Arguments:
- resid: bfloat16 [3072, 2048], P(('sp', 'tp')), may hold values from -6 to 6
- queries: bfloat16 [3072, 2048], P('sp', 'tp'), may hold values from -8 to 8
- keys: bfloat16 [3072, 512], P('sp', 'tp'), may hold values from -8 to 8
- values: bfloat16 [3072, 512], P('sp', 'tp'), may hold values from -6 to 6
- log_gates: float32 [3072, 32], P('sp', 'tp'), may hold values from -1536 to 0, as said below
- out_gate: bfloat16 [3072, 2048], P('sp', 'tp'), may hold values from -8 to 8
- out_weight: bfloat16 [2048, 2048], P('tp'), may hold values from -0.125 to 0.125
- post_gain: float32 [2048], replicated, may hold values from 0.1 to 1.9
- pre_gain: float32 [2048], replicated, may hold values from 0.1 to 1.9
- ffn_gain: float32 [2048], replicated, may hold values from 0.1 to 1.9
- gate_weight: bfloat16 [2048, 5632], P('sp', 'tp'), may hold values from -0.125 to 0.125
- up_weight: bfloat16 [2048, 5632], P('sp', 'tp'), may hold values from -0.125 to 0.125
- down_weight: bfloat16 [5632, 2048], P('tp', 'sp'), may hold values from -0.078125 to 0.078125
Outputs:
- result: bfloat16 [3072, 2048], P(('sp', 'tp'))
The draws below stay inside these ranges and needn't reach their ends.
Inputs may be any that keep to these rules, and one draw needn't show every extreme that they name: Each head's column of log_gates never rises from one position to the next, and its first entry is at most 0.
All inputs are finite; a program needn't handle non-finite values.
Results may differ from the reference program's by a relative error of at most 0.017.
Values may be sent and summed in bfloat16 or wider, within the bound.
A program may use at most 128 MiB of HBM per device.

```python
import math
import jax
import jax.numpy as jnp
from jax import lax

D = 2048
H = 32
KV = 8
HD = 64
FF = 5632
TOK_DEV = 192
TOKENS = 3072


def base_field(key, shape):
    return jnp.clip(jax.random.normal(key, shape, jnp.float32), -4.0, 4.0)


def draw_queries(key, part):
    field = base_field(jax.random.fold_in(key, 11), (TOKENS, H * HD))
    return field.astype(jnp.bfloat16)


def draw_keys(key, part):
    field = base_field(jax.random.fold_in(key, 13), (TOKENS, KV * HD))
    return field.astype(jnp.bfloat16)


def draw_log_gates(key, part):
    keyring = jax.random.split(jax.random.fold_in(key, 17), 5)
    order = jax.random.permutation(keyring[0], H)
    slow = order >= H // 2
    rate = jnp.where(slow, 0.5 / TOKENS, 1.0 / 40.0).astype(jnp.float32)
    blocks = TOKENS // TOK_DEV
    block_factor = jnp.exp(jax.random.uniform(keyring[1], (blocks,), jnp.float32, math.log(0.4), math.log(2.5)))
    block_factor = jnp.repeat(block_factor, TOK_DEV)[:, None]
    data = jnp.exp(0.6 * jnp.clip(jax.random.normal(keyring[2], (TOKENS, H), jnp.float32), -3.0, 3.0))
    steps = -rate[None, :] * block_factor * data
    hits = jax.random.uniform(keyring[3], (TOKENS, H), jnp.float32) < 2.0 / TOKENS
    loss = jax.random.uniform(keyring[4], (TOKENS, H), jnp.float32, 0.2, 0.5)
    steps = steps + jnp.where(hits & slow[None, :], jnp.log(1.0 - loss), 0.0)
    return jnp.cumsum(steps, axis=0).astype(jnp.float32)


def block_scale(rng, extent, cuts, least, top_value):
    def one(dim, shards_of):
        draws = jax.random.uniform(jax.random.fold_in(jax.random.fold_in(rng, 6), dim), (shards_of,), jnp.float32, least / len(cuts), top_value / len(cuts))
        return jnp.repeat(jnp.exp(draws), extent[dim] // shards_of).reshape((-1,) + (1,) * (len(extent) - dim - 1))

    level = one(*cuts[0])
    for cut in cuts[1:]:
        level = level * one(*cut)
    return level


def centred(own_key, extent, deviation, reach, cuts=(), kind=jnp.bfloat16):
    level = block_scale(own_key, extent, cuts, -0.22, 0.18) if cuts else 1.0
    entries = jax.random.normal(own_key, extent, jnp.float32) * deviation * level
    return jnp.minimum(jnp.maximum(entries, -reach), reach).astype(kind)


def setup_inputs(seed: int = 0) -> dict:
    seeds = jax.random.split(jax.random.key(seed), 14)
    return {
        "resid": centred(seeds[0], (TOKENS, D), 1.0, 6.0, ((0, 32),)),
        "queries": draw_queries(jax.random.fold_in(seeds[13], 71), 0),
        "keys": draw_keys(jax.random.fold_in(seeds[13], 71), 0),
        "values": centred(seeds[3], (TOKENS, KV * HD), 1.0, 6.0, ((0, 16), (1, 2))),
        "log_gates": draw_log_gates(jax.random.fold_in(seeds[13], 71), 0),
        "out_gate": centred(seeds[5], (TOKENS, H * HD), 1.5, 8.0, ((0, 16), (1, 2))),
        "out_weight": centred(seeds[6], (H * HD, D), (H * HD) ** -0.5, 0.125, ((0, 2),)),
        "post_gain": jnp.clip(1.0 + 0.18 * jax.random.normal(seeds[7], (D,), jnp.float32), 0.1, 1.9),
        "pre_gain": jnp.clip(1.0 + 0.18 * jax.random.normal(seeds[8], (D,), jnp.float32), 0.1, 1.9),
        "ffn_gain": jnp.clip(1.0 + 0.18 * jax.random.normal(seeds[9], (D,), jnp.float32), 0.1, 1.9),
        "gate_weight": centred(seeds[10], (D, FF), D ** -0.5, 0.125, ((0, 16), (1, 2))),
        "up_weight": centred(seeds[11], (D, FF), D ** -0.5, 0.125, ((0, 16), (1, 2))),
        "down_weight": centred(seeds[12], (FF, D), FF ** -0.5, 0.078125, ((0, 2), (1, 16))),
    }


EPS = 1e-06
QUERY_BLOCK = 512

def rms_scale(rows, gain):
    mean_sq = lax.optimization_barrier(jnp.mean(rows * rows, axis=-1, keepdims=True))
    return rows * lax.rsqrt(mean_sq + EPS) * gain

def reference(resid, queries, keys, values, log_gates, out_gate, out_weight, post_gain, pre_gain, ffn_gain, gate_weight, up_weight, down_weight):
    group = H // KV
    scale = HD ** (-0.5)
    total = queries.shape[0]

    def one_head(head):
        kv_head = head // group
        q_head = lax.dynamic_slice_in_dim(queries, (head * HD).astype(jnp.int32), HD, 1)
        k_head = lax.dynamic_slice_in_dim(keys, (kv_head * HD).astype(jnp.int32), HD, 1)
        v_head = lax.dynamic_slice_in_dim(values, (kv_head * HD).astype(jnp.int32), HD, 1)
        c_head = lax.dynamic_slice_in_dim(log_gates, head.astype(jnp.int32), 1, 1)[:, 0]
        pieces = []
        for first in range(0, total, QUERY_BLOCK):
            end = min(first + QUERY_BLOCK, total)
            count = end - first
            scores = jnp.dot(q_head[first:end], k_head[:end].T, preferred_element_type=jnp.float32) * scale
            scores = scores + c_head[first:end, None] - c_head[None, :end]
            causal = (first + jnp.arange(count))[:, None] >= jnp.arange(end)[None, :]
            scores = jnp.where(causal, scores, -jnp.inf)
            top = lax.optimization_barrier(jnp.max(scores, axis=1, keepdims=True))
            weights = jnp.exp(scores - top)
            denom = lax.optimization_barrier(jnp.sum(weights, axis=1, keepdims=True))
            pieces.append(jnp.dot(weights.astype(jnp.bfloat16), v_head[:end], preferred_element_type=jnp.float32) / denom)
        return jnp.concatenate(pieces, axis=0)
    attended = lax.map(one_head, jnp.arange(H, dtype=jnp.int32))
    attended = attended.transpose(1, 0, 2).reshape(total, H * HD)
    gated = (attended * jax.nn.sigmoid(out_gate.astype(jnp.float32))).astype(jnp.bfloat16)
    projected = jnp.dot(gated, out_weight, preferred_element_type=jnp.float32)
    mixed = resid.astype(jnp.float32) + rms_scale(projected, post_gain)
    normed = rms_scale(mixed, pre_gain).astype(jnp.bfloat16)
    gate = jnp.dot(normed, gate_weight, preferred_element_type=jnp.float32)
    up = jnp.dot(normed, up_weight, preferred_element_type=jnp.float32)
    hidden = (jax.nn.silu(gate) * up).astype(jnp.bfloat16)
    ffn = jnp.dot(hidden, down_weight, preferred_element_type=jnp.float32)
    return (mixed + rms_scale(ffn, ffn_gain)).astype(jnp.bfloat16)
```

```python
import functools

import jax
import jax.numpy as jnp
from jax import lax
from jax.experimental import pallas as pl
from jax.experimental.pallas import tpu as pltpu
from jax.sharding import PartitionSpec as P

HD = 64


EPS = 1e-06
KEY_BLOCK = 512


def rms_scale(rows, gain):
    mean_sq = jnp.mean(rows * rows, axis=-1, keepdims=True)
    return rows * lax.rsqrt(mean_sq + EPS) * gain


def shards(
    resid,
    queries,
    keys,
    values,
    log_gates,
    out_gate,
    out_weight,
    post_gain,
    pre_gain,
    ffn_gain,
    gate_weight,
    up_weight,
    down_weight,
):
    rows = queries.shape[0]
    head_size = HD
    kv_local = keys.shape[1] // head_size
    q_local = queries.shape[1] // head_size
    group = q_local // kv_local
    scale = head_size ** (-0.5)
    offset = lax.axis_index("sp") * rows
    last = offset + rows - 1
    query_pos = offset + jnp.arange(rows, dtype=jnp.int32)
    key_gates = lax.all_gather(log_gates, "sp", axis=0, tiled=True)
    query_blocks = queries.reshape(rows, kv_local, group, head_size)
    query_gates = log_gates.reshape(rows, kv_local, group).transpose(1, 2, 0)

    def key_block(carry, key_rows, value_rows, start):
        count = key_rows.shape[0]

        def compute(state):
            top, denom, accum = state
            scores = (
                jnp.einsum(
                    "tkgd,skd->kgts",
                    query_blocks,
                    key_rows.reshape(count, kv_local, head_size),
                    preferred_element_type=jnp.float32,
                )
                * scale
            )
            gates_here = (
                lax.dynamic_slice_in_dim(key_gates, start, count, 0)
                .reshape(count, kv_local, group)
                .transpose(1, 2, 0)
            )
            scores = scores + query_gates[:, :, :, None] - gates_here[:, :, None, :]
            causal = (start + jnp.arange(count, dtype=jnp.int32))[None, :] <= query_pos[:, None]
            scores = jnp.where(causal[None, None], scores, -jnp.inf)
            new_top = jnp.maximum(top, jnp.max(scores, axis=-1))
            shrink = jnp.exp(top - new_top)
            weights = jnp.exp(scores - new_top[..., None])
            denom = denom * shrink + jnp.sum(weights, axis=-1)
            accum = accum * shrink[..., None] + jnp.einsum(
                "kgts,skd->kgtd",
                weights.astype(jnp.bfloat16),
                value_rows.reshape(count, kv_local, head_size),
                preferred_element_type=jnp.float32,
            )
            return (new_top, denom, accum)

        def keep(state):
            return state

        return lax.cond(start <= last, compute, keep, carry)

    start_state = (
        jnp.full((kv_local, group, rows), -1e30, jnp.float32),
        jnp.zeros((kv_local, group, rows), jnp.float32),
        jnp.zeros((kv_local, group, rows, head_size), jnp.float32),
    )
    carry = start_state
    key_rows = lax.all_gather(keys, "sp", axis=0, tiled=True)
    value_rows = lax.all_gather(values, "sp", axis=0, tiled=True)
    count = key_rows.shape[0]
    blocks = count // KEY_BLOCK
    key_split = key_rows.reshape(blocks, KEY_BLOCK, key_rows.shape[1])
    value_split = value_rows.reshape(blocks, KEY_BLOCK, value_rows.shape[1])

    def advance(state, item):
        index, key_part, value_part = item
        return (key_block(state, key_part, value_part, index * KEY_BLOCK), None)

    carry, _ = lax.scan(
        advance, carry, (jnp.arange(blocks, dtype=jnp.int32), key_split, value_split)
    )
    top, denom, accum = carry
    attended = (accum / denom[..., None]).transpose(2, 0, 1, 3).reshape(rows, q_local * head_size)
    gated = (attended * jax.nn.sigmoid(out_gate.astype(jnp.float32))).astype(jnp.bfloat16)
    projected = lax.psum_scatter(
        jnp.dot(gated, out_weight, preferred_element_type=jnp.float32).astype(jnp.bfloat16),
        "tp",
        scatter_dimension=0,
        tiled=True,
    ).astype(jnp.float32)
    mixed = resid.astype(jnp.float32) + rms_scale(projected, post_gain)
    normed = rms_scale(mixed, pre_gain).astype(jnp.bfloat16)
    normed_all = lax.all_gather(normed, "tp", axis=0, tiled=True)
    gate = jnp.dot(
        normed_all,
        lax.all_gather(gate_weight, "sp", axis=0, tiled=True),
        preferred_element_type=jnp.float32,
    )
    up = jnp.dot(
        normed_all,
        lax.all_gather(up_weight, "sp", axis=0, tiled=True),
        preferred_element_type=jnp.float32,
    )
    hidden = (jax.nn.silu(gate) * up).astype(jnp.bfloat16)
    ffn_partial = jnp.dot(
        hidden,
        lax.all_gather(down_weight, "sp", axis=1, tiled=True),
        preferred_element_type=jnp.float32,
    )
    ffn = lax.psum_scatter(
        ffn_partial.astype(jnp.bfloat16), "tp", scatter_dimension=0, tiled=True
    ).astype(jnp.float32)
    return (mixed + rms_scale(ffn, ffn_gain)).astype(jnp.bfloat16)


MESH = pl.DeviceIdType.MESH
ANY = pl.BlockSpec(memory_space=pl.ANY)


def to(peer):
    return {"sp": peer}


def greet(peers):
    barrier = pltpu.get_barrier_semaphore()
    for peer in peers:
        pl.semaphore_signal(barrier, inc=1, device_id=peer, device_id_type=MESH)
    pl.semaphore_wait(barrier, len(peers))


def remote(src, dst, send, recv, peer):
    return pltpu.make_async_remote_copy(
        src_ref=src, dst_ref=dst, send_sem=send, recv_sem=recv, device_id=peer, device_id_type=MESH
    )


def swap_kernel(n, groups, x_ref, o_ref, send, recv, local):
    me = lax.axis_index("sp")
    size = n // groups
    slot = lax.rem(me, size)
    base = me - slot
    peers = [base + lax.rem(slot + j, size) for j in range(1, size)]
    greet([to(p) for p in peers])
    copies = []
    for j, p in enumerate(peers):
        c = remote(x_ref.at[p - base], o_ref.at[slot], send.at[j], recv.at[j], to(p))
        c.start()
        copies.append(c)
    own = pltpu.make_async_copy(x_ref.at[slot], o_ref.at[slot], local)
    own.start()
    own.wait()
    for c in copies:
        c.wait()


def swap(x, n, groups, cid):
    size = n // groups
    return pl.pallas_call(
        functools.partial(swap_kernel, n, groups),
        out_shape=jax.ShapeDtypeStruct(x.shape, x.dtype),
        in_specs=[ANY],
        out_specs=ANY,
        scratch_shapes=[
            pltpu.SemaphoreType.DMA((size - 1,)),
            pltpu.SemaphoreType.DMA((size - 1,)),
            pltpu.SemaphoreType.DMA,
        ],
        compiler_params=pltpu.CompilerParams(collective_id=cid, has_side_effects=True),
    )(x)


def partner_kernel(x_ref, o_ref, send, recv):
    other = 1 - lax.axis_index("tp")
    peer = {"tp": other}
    greet([peer])
    c = remote(x_ref.at[other], o_ref, send, recv, peer)
    c.start()
    c.wait()


def partner(x, cid):
    return pl.pallas_call(
        partner_kernel,
        out_shape=jax.ShapeDtypeStruct(x.shape[1:], x.dtype),
        in_specs=[ANY],
        out_specs=ANY,
        scratch_shapes=[pltpu.SemaphoreType.DMA, pltpu.SemaphoreType.DMA],
        compiler_params=pltpu.CompilerParams(collective_id=cid, has_side_effects=True),
    )(x)


def spread_kernel(n, groups, rows_ref, g_ref, u_ref, d_ref, all_ref, go_ref, uo_ref, do_ref,
                  wsend, wrecv, wlocal, asend, arecv, psend, precv, alocal):
    me = lax.axis_index("sp")
    core = lax.axis_index("tp")
    size = n // groups
    slot = lax.rem(me, size)
    base = me - slot
    mate = {"tp": 1 - core}
    order = [lax.rem(me + j, n) for j in range(1, n)]
    greet([mate] + [to(p) for p in order])
    pushes = []
    for j in range(1, size):
        c = remote(rows_ref, all_ref.at[core, slot], asend.at[j - 1], arecv.at[j - 1],
                   to(base + lax.rem(slot + j, size)))
        c.start()
        pushes.append(c)
    relays = [remote(rows_ref, all_ref.at[core, slot], psend.at[0], precv.at[0], mate)]
    relays[0].start()
    own = pltpu.make_async_copy(rows_ref, all_ref.at[core, slot], alocal)
    own.start()
    weights = []
    parts = ((g_ref, go_ref), (u_ref, uo_ref), (d_ref, do_ref))
    for j, p in enumerate(order):
        for k, (src, dst) in enumerate(parts):
            c = remote(src.at[lax.rem(p, size)], dst.at[me], wsend.at[k, j], wrecv.at[k, j], to(p))
            c.start()
            weights.append(c)
    locals_ = [pltpu.make_async_copy(src.at[slot], dst.at[me], wlocal.at[k])
               for k, (src, dst) in enumerate(parts)]
    for c in locals_:
        c.start()
    for j in range(1, size):
        pushes[j - 1].wait()
        origin = lax.rem(slot + size - j, size)
        c = remote(all_ref.at[core, origin], all_ref.at[core, origin], psend.at[j], precv.at[j], mate)
        c.start()
        relays.append(c)
    own.wait()
    for c in relays + locals_ + weights:
        c.wait()


def spread(rows, g, u, d, n, groups, cid):
    size = n // groups
    full = lambda w: jax.ShapeDtypeStruct((n,) + w.shape[1:], w.dtype)
    dma = pltpu.SemaphoreType.DMA
    return pl.pallas_call(
        functools.partial(spread_kernel, n, groups),
        out_shape=(jax.ShapeDtypeStruct((2, size) + rows.shape, rows.dtype), full(g), full(u), full(d)),
        in_specs=[ANY] * 4,
        out_specs=(ANY,) * 4,
        scratch_shapes=[
            dma((3, n - 1)), dma((3, n - 1)), dma((3,)),
            dma((size - 1,)), dma((size - 1,)), dma((size,)), dma((size,)), dma,
        ],
        compiler_params=pltpu.CompilerParams(collective_id=cid, has_side_effects=True),
    )(rows, g, u, d)


def attend_kernel(block, head, scale, q_ref, k_ref, v_ref, gc_ref, gr_ref, o_ref):
    index = pl.program_id(0)
    q = q_ref[...] * jnp.asarray(scale, q_ref.dtype)
    gc = gc_ref[...]

    def step(kb, carry, diagonal=False):
        top, acc = carry
        ks = pl.ds(pl.multiple_of(kb * block, block), block)
        s = lax.dot_general(q, k_ref[ks, :], (((1,), (1,)), ((), ())), preferred_element_type=jnp.float32)
        s = s + gc - gr_ref[:, ks]
        if diagonal:
            r = lax.broadcasted_iota(jnp.int32, s.shape, 0)
            c = lax.broadcasted_iota(jnp.int32, s.shape, 1)
            s = jnp.where(c <= r, s, -1e30)
        new = jnp.maximum(top, jnp.max(s, axis=1, keepdims=True))
        p = jnp.exp(s - new).astype(jnp.bfloat16)
        acc = acc * jnp.exp(top - new) + jnp.dot(p, v_ref[ks, :], preferred_element_type=jnp.float32)
        return new, acc

    start = (jnp.full((block, 1), -1e30, jnp.float32), jnp.zeros((block, v_ref.shape[1]), jnp.float32))
    carry = step(index, start, True)
    _, acc = lax.fori_loop(0, index, step, carry)
    o_ref[...] = (acc[:, :head] / acc[:, head:head + 1]).astype(o_ref.dtype)


def attend(q, k, v, gates, block):
    total, head = q.shape
    whole = lambda a: pl.BlockSpec(a.shape, lambda i: (0, 0))
    row = gates.reshape(1, total)
    return pl.pallas_call(
        functools.partial(attend_kernel, block, head, head ** -0.5),
        grid=(total // block,),
        out_shape=jax.ShapeDtypeStruct((total, head), jnp.bfloat16),
        in_specs=[
            pl.BlockSpec((block, head), lambda i: (i, 0)), whole(k), whole(v),
            pl.BlockSpec((block, 1), lambda i: (i, 0)), whole(row),
        ],
        out_specs=pl.BlockSpec((block, head), lambda i: (i, 0)),
        compiler_params=pltpu.CompilerParams(
            dimension_semantics=("arbitrary",), vmem_limit_bytes=40 * 1024 * 1024
        ),
    )(q, k, v, gates.reshape(total, 1), row)


def halves(x, lanes):
    *lead, r, h = x.shape
    f = lanes // h
    x = x.reshape(*lead, f, r // f, h)
    return jnp.swapaxes(x, -3, -2).reshape(*lead, r // f, lanes)


def unhalves(x, h):
    *lead, r, lanes = x.shape
    f = lanes // h
    x = x.reshape(*lead, r, f, h)
    return jnp.swapaxes(x, -3, -2).reshape(*lead, r * f, h)


LANES = 128


def pack(queries, keys, values, log_gates, heads):
    rows = queries.shape[0]
    kv = keys.shape[1] // HD
    group = heads // kv
    by_head = lambda a, m: jnp.repeat(a.reshape(rows, m, HD).transpose(1, 0, 2), heads // m, axis=0)
    qk = jnp.concatenate([by_head(queries, heads), by_head(keys, kv)], axis=-1)
    v = jnp.repeat(halves(values.reshape(rows, kv, HD).transpose(1, 0, 2), LANES), group, axis=0)
    g = log_gates.T
    hi = lax.reduce_precision(g, 8, 7)
    mid = lax.reduce_precision(g - hi, 8, 7)
    low = g - hi - mid
    g3 = jnp.stack([hi, mid, low], axis=1).reshape(heads, 3 * rows)
    pad = -(3 * rows) % (16 * LANES)
    g3 = jnp.pad(g3, ((0, 0), (0, pad))).reshape(heads, -1, LANES).astype(jnp.bfloat16)
    return jnp.concatenate([qk, v, g3], axis=1)


def unpack(got, rows):
    n = got.shape[0]
    qk = got[:, :rows].reshape(n * rows, 2 * HD)
    v = unhalves(got[:, rows:rows + rows * HD // LANES], HD).reshape(n * rows, HD)
    g3 = got[:, rows + rows * HD // LANES:].reshape(n, -1)[:, :3 * rows].reshape(n, 3, rows)
    g3 = g3.astype(jnp.float32)
    gates = (g3[:, 0] + g3[:, 1]) + g3[:, 2]
    v = jnp.concatenate([v, jnp.ones_like(v)], axis=1)
    return qk[:, :HD], qk[:, HD:], v, gates.reshape(n * rows)


def fast_shards(n, resid, queries, keys, values, log_gates, out_gate, out_weight, post_gain,
                pre_gain, ffn_gain, gate_weight, up_weight, down_weight):
    rows = queries.shape[0]
    heads = queries.shape[1] // HD
    width = resid.shape[1]
    groups = 2
    size = n // groups
    ff = gate_weight.shape[1] // size
    got = swap(pack(queries, keys, values, log_gates, heads), n, 1, 1)
    q, k, v, gates = unpack(got, rows)
    att = attend(q, k, v, gates, n * rows // 6)
    back = swap(halves(att.reshape(n, rows, HD), LANES), n, 1, 2)
    attended = unhalves(back, HD).transpose(1, 0, 2).reshape(rows, heads * HD).astype(jnp.float32)
    gated = (attended * jax.nn.sigmoid(out_gate.astype(jnp.float32))).astype(jnp.bfloat16)
    partial = jnp.dot(gated, out_weight, preferred_element_type=jnp.float32)
    core = lax.axis_index("tp")
    partial = partial.astype(jnp.bfloat16).reshape(2, rows // 2, width)
    mine = lambda a: lax.dynamic_index_in_dim(a, core, 0, keepdims=False).astype(jnp.float32)
    projected = mine(partial) + partner(partial, 3).astype(jnp.float32)
    mixed = resid.astype(jnp.float32) + rms_scale(projected, post_gain)
    normed = rms_scale(mixed, pre_gain).astype(jnp.bfloat16)
    cut = lambda w: w.reshape(w.shape[0], size, ff).transpose(1, 0, 2)
    normed_all, gw, uw, dw = spread(
        normed, cut(gate_weight), cut(up_weight), down_weight.reshape(size, ff, -1), n, groups, 4
    )
    x = normed_all.reshape(2 * size * normed.shape[0], width)
    gate = jnp.dot(x, gw.reshape(width, ff), preferred_element_type=jnp.float32)
    up = jnp.dot(x, uw.reshape(width, ff), preferred_element_type=jnp.float32)
    hidden = (jax.nn.silu(gate) * up).astype(jnp.bfloat16)
    down = dw.transpose(1, 0, 2).reshape(ff, width)
    part = jnp.dot(hidden, down, preferred_element_type=jnp.float32).astype(jnp.bfloat16)
    part = part.reshape(2, size * normed.shape[0], width)
    both = mine(part) + partner(part, 5).astype(jnp.float32)
    both = both.astype(jnp.bfloat16).reshape(size, normed.shape[0], width)
    ffn = jnp.sum(swap(both, n, groups, 6).astype(jnp.float32), axis=0)
    return (mixed + rms_scale(ffn, ffn_gain)).astype(jnp.bfloat16)


def solution(mesh):
    n, cores = mesh.shape["sp"], mesh.shape["tp"]

    def body(*args):
        queries, gate_weight = args[1], args[10]
        fits = cores == 2 and queries.shape[1] == n * HD and n % 2 == 0
        fits = fits and gate_weight.shape[1] % (n * 8) == 0
        return fast_shards(n, *args) if fits else shards(*args)

    in_specs = (
        P(("sp", "tp"), None),
        P("sp", "tp"),
        P("sp", "tp"),
        P("sp", "tp"),
        P("sp", "tp"),
        P("sp", "tp"),
        P("tp", None),
        P(),
        P(),
        P(),
        P("sp", "tp"),
        P("sp", "tp"),
        P("tp", "sp"),
    )
    out_specs = P(("sp", "tp"), None)
    return jax.shard_map(body, mesh=mesh, in_specs=in_specs, out_specs=out_specs, check_vma=False)
```

```python
import functools

import jax
import jax.numpy as jnp
from jax import lax
from jax.experimental import pallas as pl
from jax.experimental.layout import Layout, with_layout_constraint
from jax.experimental.pallas import tpu as pltpu
from jax.sharding import PartitionSpec as P


HD = 64


EPS = 1e-06
KEY_BLOCK = 512


def rms_scale(rows, gain):
    mean_sq = jnp.mean(rows * rows, axis=-1, keepdims=True)
    return rows * lax.rsqrt(mean_sq + EPS) * gain


def shards(
    resid,
    queries,
    keys,
    values,
    log_gates,
    out_gate,
    out_weight,
    post_gain,
    pre_gain,
    ffn_gain,
    gate_weight,
    up_weight,
    down_weight,
):
    rows = queries.shape[0]
    head_size = HD
    kv_local = keys.shape[1] // head_size
    q_local = queries.shape[1] // head_size
    group = q_local // kv_local
    scale = head_size ** (-0.5)
    offset = lax.axis_index("sp") * rows
    last = offset + rows - 1
    query_pos = offset + jnp.arange(rows, dtype=jnp.int32)
    key_gates = lax.all_gather(log_gates, "sp", axis=0, tiled=True)
    query_blocks = queries.reshape(rows, kv_local, group, head_size)
    query_gates = log_gates.reshape(rows, kv_local, group).transpose(1, 2, 0)

    def key_block(carry, key_rows, value_rows, start):
        count = key_rows.shape[0]

        def compute(state):
            top, denom, accum = state
            scores = (
                jnp.einsum(
                    "tkgd,skd->kgts",
                    query_blocks,
                    key_rows.reshape(count, kv_local, head_size),
                    preferred_element_type=jnp.float32,
                )
                * scale
            )
            gates_here = (
                lax.dynamic_slice_in_dim(key_gates, start, count, 0)
                .reshape(count, kv_local, group)
                .transpose(1, 2, 0)
            )
            scores = scores + query_gates[:, :, :, None] - gates_here[:, :, None, :]
            causal = (start + jnp.arange(count, dtype=jnp.int32))[None, :] <= query_pos[:, None]
            scores = jnp.where(causal[None, None], scores, -jnp.inf)
            new_top = jnp.maximum(top, jnp.max(scores, axis=-1))
            shrink = jnp.exp(top - new_top)
            weights = jnp.exp(scores - new_top[..., None])
            denom = denom * shrink + jnp.sum(weights, axis=-1)
            accum = accum * shrink[..., None] + jnp.einsum(
                "kgts,skd->kgtd",
                weights.astype(jnp.bfloat16),
                value_rows.reshape(count, kv_local, head_size),
                preferred_element_type=jnp.float32,
            )
            return (new_top, denom, accum)

        def keep(state):
            return state

        return lax.cond(start <= last, compute, keep, carry)

    start_state = (
        jnp.full((kv_local, group, rows), -1e30, jnp.float32),
        jnp.zeros((kv_local, group, rows), jnp.float32),
        jnp.zeros((kv_local, group, rows, head_size), jnp.float32),
    )
    carry = start_state
    key_rows = lax.all_gather(keys, "sp", axis=0, tiled=True)
    value_rows = lax.all_gather(values, "sp", axis=0, tiled=True)
    count = key_rows.shape[0]
    blocks = count // KEY_BLOCK
    key_split = key_rows.reshape(blocks, KEY_BLOCK, key_rows.shape[1])
    value_split = value_rows.reshape(blocks, KEY_BLOCK, value_rows.shape[1])

    def advance(state, item):
        index, key_part, value_part = item
        return (key_block(state, key_part, value_part, index * KEY_BLOCK), None)

    carry, _ = lax.scan(
        advance, carry, (jnp.arange(blocks, dtype=jnp.int32), key_split, value_split)
    )
    _, denom, accum = carry
    attended = (accum / denom[..., None]).transpose(2, 0, 1, 3).reshape(rows, q_local * head_size)
    gated = (attended * jax.nn.sigmoid(out_gate.astype(jnp.float32))).astype(jnp.bfloat16)
    projected = lax.psum_scatter(
        jnp.dot(gated, out_weight, preferred_element_type=jnp.float32).astype(jnp.bfloat16),
        "tp",
        scatter_dimension=0,
        tiled=True,
    ).astype(jnp.float32)
    mixed = resid.astype(jnp.float32) + rms_scale(projected, post_gain)
    normed = rms_scale(mixed, pre_gain).astype(jnp.bfloat16)
    normed_all = lax.all_gather(normed, "tp", axis=0, tiled=True)
    gate = jnp.dot(
        normed_all,
        lax.all_gather(gate_weight, "sp", axis=0, tiled=True),
        preferred_element_type=jnp.float32,
    )
    up = jnp.dot(
        normed_all,
        lax.all_gather(up_weight, "sp", axis=0, tiled=True),
        preferred_element_type=jnp.float32,
    )
    hidden = (jax.nn.silu(gate) * up).astype(jnp.bfloat16)
    ffn_partial = jnp.dot(
        hidden,
        lax.all_gather(down_weight, "sp", axis=1, tiled=True),
        preferred_element_type=jnp.float32,
    )
    ffn = lax.psum_scatter(
        ffn_partial.astype(jnp.bfloat16), "tp", scatter_dimension=0, tiled=True
    ).astype(jnp.float32)
    return (mixed + rms_scale(ffn, ffn_gain)).astype(jnp.bfloat16)


MESH = pl.DeviceIdType.MESH
ANY = pl.BlockSpec(memory_space=pl.ANY)


def to(peer):
    return {"sp": peer}


def greet(peers):
    barrier = pltpu.get_barrier_semaphore()
    for peer in peers:
        pl.semaphore_signal(barrier, inc=1, device_id=peer, device_id_type=MESH)
    pl.semaphore_wait(barrier, len(peers))


def remote(src, dst, send, recv, peer):
    return pltpu.make_async_remote_copy(
        src_ref=src, dst_ref=dst, send_sem=send, recv_sem=recv, device_id=peer, device_id_type=MESH
    )


def mixed_order(size):
    order = []
    for j in range(1, size // 2 + 1):
        order += [k for k in (size - 1 - j, j) if k and k not in order]
    return order + [k for k in range(1, size) if k not in order]


def swap_kernel(n, groups, x_ref, o_ref, send, recv, local):
    me = lax.axis_index("sp")
    size = n // groups
    slot = lax.rem(me, size)
    base = me - slot
    peers = [base + (slot ^ j) for j in mixed_order(size)]
    greet([to(p) for p in peers])
    copies = []
    for j, p in enumerate(peers):
        c = remote(x_ref.at[p - base], o_ref.at[slot], send.at[j], recv.at[j], to(p))
        c.start()
        copies.append(c)
    own = pltpu.make_async_copy(x_ref.at[slot], o_ref.at[slot], local)
    own.start()
    own.wait()
    for c in copies:
        c.wait()


def swap(x, n, groups, cid):
    size = n // groups
    return pl.pallas_call(
        functools.partial(swap_kernel, n, groups),
        out_shape=jax.ShapeDtypeStruct(x.shape, x.dtype),
        in_specs=[ANY],
        out_specs=ANY,
        scratch_shapes=[
            pltpu.SemaphoreType.DMA((size - 1,)),
            pltpu.SemaphoreType.DMA((size - 1,)),
            pltpu.SemaphoreType.DMA,
        ],
        compiler_params=pltpu.CompilerParams(collective_id=cid, has_side_effects=True),
    )(x)


def partner_kernel(x_ref, o_ref, send, recv):
    other = 1 - lax.axis_index("tp")
    peer = {"tp": other}
    greet([peer])
    c = remote(x_ref.at[other], o_ref, send, recv, peer)
    c.start()
    c.wait()


def partner(x, cid):
    return pl.pallas_call(
        partner_kernel,
        out_shape=jax.ShapeDtypeStruct(x.shape[1:], x.dtype),
        in_specs=[ANY],
        out_specs=ANY,
        scratch_shapes=[pltpu.SemaphoreType.DMA, pltpu.SemaphoreType.DMA],
        compiler_params=pltpu.CompilerParams(collective_id=cid, has_side_effects=True),
    )(x)


def spread_kernel(n, groups, rows_ref, all_ref, asend, arecv, psend, precv, alocal):
    me = lax.axis_index("sp")
    core = lax.axis_index("tp")
    size = n // groups
    slot = lax.rem(me, size)
    base = me - slot
    mate = {"tp": 1 - core}
    others = [slot ^ j for j in mixed_order(size)]
    greet([mate] + [to(base + p) for p in others])
    mine = all_ref.at[core, slot]
    relays = [remote(rows_ref, mine, psend.at[0], precv.at[0], mate)]
    relays[0].start()
    pushes = []
    for j, p in enumerate(others):
        c = remote(rows_ref, mine, asend.at[j], arecv.at[j], to(base + p))
        c.start()
        pushes.append(c)
    own = pltpu.make_async_copy(rows_ref, mine, alocal)
    own.start()
    for j, p in enumerate(others):
        pushes[j].wait_recv()
        c = remote(all_ref.at[core, p], all_ref.at[core, p], psend.at[j + 1], precv.at[j + 1], mate)
        c.start()
        relays.append(c)
    own.wait()
    for c in pushes:
        c.wait_send()
    for c in relays:
        c.wait()


def spread(rows, n, groups, cid):
    size = n // groups
    dma = pltpu.SemaphoreType.DMA
    return pl.pallas_call(
        functools.partial(spread_kernel, n, groups),
        out_shape=jax.ShapeDtypeStruct((2, size) + rows.shape, rows.dtype),
        in_specs=[ANY],
        out_specs=ANY,
        scratch_shapes=[dma((size - 1,)), dma((size - 1,)), dma((size,)), dma((size,)), dma],
        compiler_params=pltpu.CompilerParams(collective_id=cid, has_side_effects=True),
    )(rows)


def hidden_blocks(gate_weight, up_weight, down_weight, size):
    ff = gate_weight.shape[1] // size
    cut = lambda w: w.reshape(w.shape[0], size, ff).transpose(1, 0, 2)
    blocks = jnp.stack([cut(gate_weight), cut(up_weight), cut(down_weight.T)], axis=1)
    return with_layout_constraint(blocks, Layout(major_to_minor=(0, 1, 2, 3)))


def ship(blocks, shifts, n, after):
    me = lax.axis_index("sp")
    blocks, after = lax.optimization_barrier((blocks, after))
    arrived = {}
    for j in shifts:
        got = lax.dynamic_index_in_dim(blocks, lax.rem(me ^ j, blocks.shape[0]), 0, keepdims=False)
        got = with_layout_constraint(got, Layout(major_to_minor=(0, 1, 2)))
        arrived[j] = lax.ppermute(got, "sp", [(i, i ^ j) for i in range(n)])
    return arrived, after


def collect_kernel(shifts, *refs):
    *arrived, out_ref, sems = refs
    me = lax.axis_index("sp")
    copies = []
    for i, (j, src) in enumerate(zip(shifts, arrived)):
        copies += [pltpu.make_async_copy(src.at[k], out_ref.at[k, me ^ j], sems.at[i, k])
                   for k in range(src.shape[0])]
    for c in copies:
        c.start()
    for c in copies:
        c.wait()


def collect(blocks, arrived, n):
    me = lax.axis_index("sp")
    own = lax.dynamic_index_in_dim(blocks, lax.rem(me, blocks.shape[0]), 0, keepdims=False)
    arrived = {0: own, **arrived}
    kinds = own.shape[0]
    return pl.pallas_call(
        functools.partial(collect_kernel, tuple(arrived)),
        out_shape=jax.ShapeDtypeStruct((kinds, n) + own.shape[1:], own.dtype),
        in_specs=[ANY] * len(arrived),
        out_specs=pl.BlockSpec(memory_space=pltpu.VMEM),
        scratch_shapes=[pltpu.SemaphoreType.DMA((len(arrived), kinds))],
        compiler_params=pltpu.CompilerParams(vmem_limit_bytes=32 * 1024 * 1024),
    )(*arrived.values())


def attend_kernel(block, head, scale, q_ref, k_ref, v_ref, gc_ref, gr_ref, o_ref):
    index = pl.program_id(0)
    q = q_ref[...] * jnp.asarray(scale, q_ref.dtype)
    gc = gc_ref[...]

    def step(kb, carry, diagonal=False):
        top, acc = carry
        ks = pl.ds(pl.multiple_of(kb * block, block), block)
        s = lax.dot_general(q, k_ref[ks, :], (((1,), (1,)), ((), ())), preferred_element_type=jnp.float32)
        s = s + gc - gr_ref[:, ks]
        if diagonal:
            r = lax.broadcasted_iota(jnp.int32, s.shape, 0)
            c = lax.broadcasted_iota(jnp.int32, s.shape, 1)
            s = jnp.where(c <= r, s, -1e30)
        new = jnp.maximum(top, jnp.max(s, axis=1, keepdims=True))
        p = jnp.exp(s - new).astype(jnp.bfloat16)
        acc = acc * jnp.exp(top - new) + jnp.dot(p, v_ref[ks, :], preferred_element_type=jnp.float32)
        return new, acc

    start = (jnp.full((block, 1), -1e30, jnp.float32), jnp.zeros((block, v_ref.shape[1]), jnp.float32))
    carry = step(index, start, True)
    _, acc = lax.fori_loop(0, index, step, carry)
    o_ref[...] = (acc[:, :head] / acc[:, head:head + 1]).astype(o_ref.dtype)


def attend(q, k, v, gates, block):
    total, head = q.shape
    whole = lambda a: pl.BlockSpec(a.shape, lambda i: (0, 0))
    row = gates.reshape(1, total)
    return pl.pallas_call(
        functools.partial(attend_kernel, block, head, head ** -0.5),
        grid=(total // block,),
        out_shape=jax.ShapeDtypeStruct((total, head), jnp.bfloat16),
        in_specs=[
            pl.BlockSpec((block, head), lambda i: (i, 0)), whole(k), whole(v),
            pl.BlockSpec((block, 1), lambda i: (i, 0)), whole(row),
        ],
        out_specs=pl.BlockSpec((block, head), lambda i: (i, 0)),
        compiler_params=pltpu.CompilerParams(
            dimension_semantics=("arbitrary",), vmem_limit_bytes=40 * 1024 * 1024
        ),
    )(q, k, v, gates.reshape(total, 1), row)


def halves(x, lanes):
    *lead, r, h = x.shape
    f = lanes // h
    x = x.reshape(*lead, f, r // f, h)
    return jnp.swapaxes(x, -3, -2).reshape(*lead, r // f, lanes)


def unhalves(x, h):
    *lead, r, lanes = x.shape
    f = lanes // h
    x = x.reshape(*lead, r, f, h)
    return jnp.swapaxes(x, -3, -2).reshape(*lead, r * f, h)


LANES = 128


def pack(queries, keys, values, log_gates, heads):
    rows = queries.shape[0]
    kv = keys.shape[1] // HD
    group = heads // kv
    by_head = lambda a, m: jnp.repeat(a.reshape(rows, m, HD).transpose(1, 0, 2), heads // m, axis=0)
    qk = jnp.concatenate([by_head(queries, heads), by_head(keys, kv)], axis=-1)
    v = jnp.repeat(halves(values.reshape(rows, kv, HD).transpose(1, 0, 2), LANES), group, axis=0)
    g = log_gates.T
    hi = lax.reduce_precision(g, 8, 7)
    mid = lax.reduce_precision(g - hi, 8, 7)
    low = g - hi - mid
    g3 = jnp.stack([hi, mid, low], axis=1).reshape(heads, 3 * rows)
    pad = -(3 * rows) % (16 * LANES)
    g3 = jnp.pad(g3, ((0, 0), (0, pad))).reshape(heads, -1, LANES).astype(jnp.bfloat16)
    return jnp.concatenate([qk, v, g3], axis=1)


def unpack(got, rows):
    n = got.shape[0]
    qk = got[:, :rows].reshape(n * rows, 2 * HD)
    v = unhalves(got[:, rows:rows + rows * HD // LANES], HD).reshape(n * rows, HD)
    g3 = got[:, rows + rows * HD // LANES:].reshape(n, -1)[:, :3 * rows].reshape(n, 3, rows)
    g3 = g3.astype(jnp.float32)
    gates = (g3[:, 0] + g3[:, 1]) + g3[:, 2]
    v = jnp.concatenate([v, jnp.ones_like(v)], axis=1)
    return qk[:, :HD], qk[:, HD:], v, gates.reshape(n * rows)


def fast_shards(n, resid, queries, keys, values, log_gates, out_gate, out_weight, post_gain,
                pre_gain, ffn_gain, gate_weight, up_weight, down_weight):
    rows = queries.shape[0]
    heads = queries.shape[1] // HD
    width = resid.shape[1]
    groups = 2
    size = n // groups
    ff = gate_weight.shape[1] // size
    blocks = hidden_blocks(gate_weight, up_weight, down_weight, size)
    got = swap(pack(queries, keys, values, log_gates, heads), n, 1, 1)
    early = list(range(size, size + 3)) + list(range(1, size))
    first, got = ship(blocks, early, n, got)
    q, k, v, gates = unpack(got, rows)
    att = attend(q, k, v, gates, n * rows // 6)
    back = swap(halves(att.reshape(n, rows, HD), LANES), n, 1, 2)
    second, back = ship(blocks, range(size + 3, n), n, back)
    attended = unhalves(back, HD).transpose(1, 0, 2).reshape(rows, heads * HD).astype(jnp.float32)
    gated = (attended * jax.nn.sigmoid(out_gate.astype(jnp.float32))).astype(jnp.bfloat16)
    partial = jnp.dot(gated, out_weight, preferred_element_type=jnp.float32)
    core = lax.axis_index("tp")
    partial = partial.astype(jnp.bfloat16).reshape(2, rows // 2, width)
    mine = lambda a: lax.dynamic_index_in_dim(a, core, 0, keepdims=False).astype(jnp.float32)
    projected = mine(partial) + partner(partial, 3).astype(jnp.float32)
    mixed = resid.astype(jnp.float32) + rms_scale(projected, post_gain)
    normed = rms_scale(mixed, pre_gain).astype(jnp.bfloat16)
    normed_all = spread(normed, n, groups, 4)
    first, second, normed_all = lax.optimization_barrier((first, second, normed_all))
    weights = collect(blocks, {**first, **second}, n)
    x = normed_all.reshape(2 * size * normed.shape[0], width)
    gw, uw, dw = [weights[i].reshape(width, ff) for i in range(3)]
    gate = jnp.dot(x, gw, preferred_element_type=jnp.float32)
    up = jnp.dot(x, uw, preferred_element_type=jnp.float32)
    hidden = (jax.nn.silu(gate) * up).astype(jnp.bfloat16)
    part = jnp.einsum("tf,df->td", hidden, dw, preferred_element_type=jnp.float32).astype(jnp.bfloat16)
    part = part.reshape(2, size * normed.shape[0], width)
    both = mine(part) + partner(part, 5).astype(jnp.float32)
    both = both.astype(jnp.bfloat16).reshape(size, normed.shape[0], width)
    ffn = jnp.sum(swap(both, n, groups, 6).astype(jnp.float32), axis=0)
    return (mixed + rms_scale(ffn, ffn_gain)).astype(jnp.bfloat16)


def solution(mesh):
    n, cores = mesh.shape["sp"], mesh.shape["tp"]

    def body(*args):
        queries, gate_weight = args[1], args[10]
        fits = cores == 2 and queries.shape[1] == n * HD and n & (n - 1) == 0
        fits = fits and gate_weight.shape[1] % (n * 8) == 0
        return fast_shards(n, *args) if fits else shards(*args)

    in_specs = (
        P(("sp", "tp"), None),
        P("sp", "tp"),
        P("sp", "tp"),
        P("sp", "tp"),
        P("sp", "tp"),
        P("sp", "tp"),
        P("tp", None),
        P(),
        P(),
        P(),
        P("sp", "tp"),
        P("sp", "tp"),
        P("tp", "sp"),
    )
    out_specs = P(("sp", "tp"), None)
    return jax.shard_map(body, mesh=mesh, in_specs=in_specs, out_specs=out_specs, check_vma=False)
```
